32 devices in a mesh: kv: 16 (over z, y, core), tp: 2 (over x).
Axes of the slice: x: 2, y: 2, z: 4, core: 2. Of those that a mesh axis runs over, the one named last changes fastest.
Arguments:
- queries: bfloat16 [4096, 1536], P('kv', 'tp'), may hold values from -6 to 6
- keys: bfloat16 [4096, 256], P('kv', 'tp'), may hold values from -6 to 6
- values: bfloat16 [4096, 256], P('kv', 'tp'), may hold values from -6 to 6
- log_sums: float32 [12, 4096], P('tp', 'kv'), may hold values from 6 to 7.5
- out_grad: bfloat16 [4096, 1536], P('kv', 'tp'), may hold values from -6 to 6
- chosen: int32 [64, 2, 8], P('kv', 'tp'), may hold values from 0 to 63, as said below
- inputs: bfloat16 [4096, 3072], P('kv', 'tp'), may hold values from -6 to 6
Outputs:
- query_grad: bfloat16 [4096, 1536], P('kv', 'tp')
- key_grad: bfloat16 [4096, 256], P('kv', 'tp')
- value_grad: bfloat16 [4096, 256], P('kv', 'tp')
- weight_grad: float32 [3072, 256], P('kv', 'tp')
The draws below stay inside these ranges and needn't reach their ends.
Inputs may be any that keep to these rules, and one draw needn't show every extreme that they name: `chosen`: for query block g and key head h, every slot holds g (an empty slot) or a key block c with g - 16 <= c < g; the blocks of the live slots of one list are distinct; each list has between 4 and 8 live slots, except that query block g has at most g of them (block 0 has none).
All inputs are finite; a program needn't handle non-finite values.
Results may differ from the reference program's by a relative error of at most 0.0049.
Values may be sent and summed in bfloat16 or wider, within the bound.
A program may use at most 64 MiB of HBM per device.

```python
import jax
import jax.numpy as jnp
from jax import lax

D = 3072
HDIM = 128
QPK = 6
BLK = 64
SEL = 8
REACH = 4
BPD = 4
KVH = 2
HEADS = 12
NBLK = 64
TOKENS = 4096


def draw_chosen(key, part):
    window_span = REACH * BPD
    order_key = jax.random.fold_in(key, 11)
    count_key = jax.random.fold_in(key, 12)
    blocks = jnp.arange(NBLK, dtype=jnp.int32)[:, None, None]
    offsets = jnp.arange(1, window_span + 1, dtype=jnp.int32)[None, None, :]
    scores = jax.random.randint(order_key, (NBLK, KVH, window_span), 0, 1 << 20, dtype=jnp.int32) * window_span + offsets - 1
    scores = jnp.where(blocks - offsets >= 0, scores, -offsets)
    top_values, picked = lax.top_k(scores, SEL)
    chosen_ids = blocks - 1 - picked.astype(jnp.int32)
    live_count = jax.random.randint(count_key, (NBLK, KVH, 1), SEL // 2, SEL + 1, dtype=jnp.int32)
    slot_index = jnp.arange(SEL, dtype=jnp.int32)[None, None, :]
    keep_mask = (slot_index < live_count) & (chosen_ids >= 0)
    return jnp.where(keep_mask, chosen_ids, blocks)


def steps_of(stream_key, shape, shards, least, largest):
    factor_of = 1.0
    for dim, parts in shards:
        steps = jax.random.uniform(jax.random.fold_in(jax.random.fold_in(stream_key, 6), dim), (parts,), jnp.float32, least / len(shards), largest / len(shards))
        factor_of = factor_of * jnp.repeat(jnp.exp(steps), shape[dim] // parts).reshape((-1,) + (1,) * (len(shape) - 1 - dim))
    return factor_of


def gaussian(stream_key, shape, width, reach, split=(), kind=jnp.bfloat16):
    level = steps_of(stream_key, shape, split, -0.22, 0.18) if split else 1.0
    entries = jax.random.normal(stream_key, shape, jnp.float32) * width * level
    return jnp.minimum(jnp.maximum(entries, -reach), reach).astype(kind)


def setup_inputs(seed: int = 0) -> dict:
    splits = jax.random.split(jax.random.key(seed), 8)
    queries = gaussian(splits[0], (TOKENS, HEADS * HDIM), 1.0, 6.0, ((0, 16), (1, 2)))
    keys = gaussian(splits[1], (TOKENS, KVH * HDIM), 1.0, 6.0, ((0, 16), (1, 2)))
    values = gaussian(splits[2], (TOKENS, KVH * HDIM), 1.0, 6.0, ((0, 16), (1, 2)))
    log_sums = jnp.clip(6.0 + 1.5 * jax.random.uniform(splits[3], (HEADS, TOKENS), jnp.float32) ** steps_of(splits[3], (HEADS, TOKENS), ((0, 2), (1, 16)), -0.2, 0.2), 6.0, 7.5)
    out_grad = gaussian(splits[4], (TOKENS, HEADS * HDIM), 1.0, 6.0, ((0, 16), (1, 2)))
    chosen = draw_chosen(jax.random.fold_in(splits[7], 71), 0)
    inputs = gaussian(splits[6], (TOKENS, D), 1.0, 6.0, ((0, 16), (1, 2)))
    return {"queries": queries, "keys": keys, "values": values, "log_sums": log_sums, "out_grad": out_grad, "chosen": chosen, "inputs": inputs}


def rounded(tensor):
    return lax.optimization_barrier(tensor.astype(jnp.bfloat16)).astype(jnp.float32)


def reference(queries, keys, values, log_sums, out_grad, chosen, inputs):
    scaling = HDIM ** -0.5
    query_tile_set = queries.reshape(NBLK, BLK, KVH, QPK, HDIM)
    gradient_tiles = out_grad.reshape(NBLK, BLK, KVH, QPK, HDIM)
    sum_tiles = log_sums.reshape(KVH, QPK, NBLK, BLK).transpose(2, 0, 1, 3)
    key_tiles = keys.reshape(NBLK, BLK, KVH, HDIM)
    value_tiles = values.reshape(NBLK, BLK, KVH, HDIM)
    head_ids = jnp.arange(KVH, dtype=jnp.int32)[:, None]
    offsets = jnp.arange(BLK, dtype=jnp.int32)
    causal = (offsets[None, :] <= offsets[:, None])[None, :, None, :]

    def visit(carry, index):
        key_acc, value_acc = carry
        listed = chosen[index]
        live_slots = listed < index
        sel_keys = key_tiles[listed, :, head_ids]
        sel_values = value_tiles[listed, :, head_ids]
        own_keys = lax.dynamic_index_in_dim(key_tiles, index, 0, keepdims=False).transpose(1, 0, 2)[:, None]
        own_values = lax.dynamic_index_in_dim(value_tiles, index, 0, keepdims=False).transpose(1, 0, 2)[:, None]
        all_keys = jnp.concatenate([sel_keys, own_keys], 1).reshape(KVH, (SEL + 1) * BLK, HDIM).astype(jnp.float32)
        all_values = jnp.concatenate([sel_values, own_values], 1).reshape(KVH, (SEL + 1) * BLK, HDIM).astype(jnp.float32)
        mask_sel = jnp.broadcast_to(live_slots[:, None, :, None], (KVH, BLK, SEL, BLK))
        mask_own = jnp.broadcast_to(causal, (KVH, BLK, 1, BLK))
        permitted_mask = jnp.concatenate([mask_sel, mask_own], 2).reshape(KVH, BLK, (SEL + 1) * BLK)
        query_rows = lax.dynamic_index_in_dim(query_tile_set, index, 0, keepdims=False).astype(jnp.float32)
        grad_rows = lax.dynamic_index_in_dim(gradient_tiles, index, 0, keepdims=False).astype(jnp.float32)
        sum_rows = lax.dynamic_index_in_dim(sum_tiles, index, 0, keepdims=False)
        scores = jnp.einsum('qhgd,hkd->hgqk', query_rows, all_keys) * scaling
        weights = jnp.where(permitted_mask[:, None], jnp.exp(scores - sum_rows[..., None]), 0.0)
        grad_weights = jnp.einsum('qhgd,hkd->hgqk', grad_rows, all_values)
        delta_rows = jnp.sum(weights * grad_weights, -1, keepdims=True)
        score_gradient = rounded(weights * (grad_weights - delta_rows))
        weights_reduced = rounded(weights)
        query_part = jnp.einsum('hgqk,hkd->qhgd', score_gradient, all_keys) * scaling
        key_part = (jnp.einsum('hgqk,qhgd->hkd', score_gradient, query_rows) * scaling).reshape(KVH, SEL + 1, BLK, HDIM)
        value_part = jnp.einsum('hgqk,qhgd->hkd', weights_reduced, grad_rows).reshape(KVH, SEL + 1, BLK, HDIM)
        key_acc = key_acc.at[listed, :, head_ids].add(key_part[:, :SEL])
        key_acc = key_acc.at[index].add(key_part[:, SEL].transpose(1, 0, 2))
        value_acc = value_acc.at[listed, :, head_ids].add(value_part[:, :SEL])
        value_acc = value_acc.at[index].add(value_part[:, SEL].transpose(1, 0, 2))
        return (key_acc, value_acc), query_part.reshape(BLK, HEADS * HDIM).astype(jnp.bfloat16)

    zeros_acc = jnp.zeros((NBLK, BLK, KVH, HDIM), jnp.float32)
    (key_acc, value_acc), query_blocks = lax.scan(visit, (zeros_acc, zeros_acc), jnp.arange(NBLK, dtype=jnp.int32))
    query_grad = query_blocks.reshape(TOKENS, HEADS * HDIM)
    key_grad = key_acc.reshape(TOKENS, KVH * HDIM).astype(jnp.bfloat16)
    value_grad = value_acc.reshape(TOKENS, KVH * HDIM).astype(jnp.bfloat16)
    weight_grad = jnp.dot(inputs.T, value_grad, preferred_element_type=jnp.float32)
    return (query_grad, key_grad, value_grad, weight_grad)
```

```python
import functools

import jax
import jax.numpy as jnp
from jax import lax
from jax.experimental import pallas as pl
from jax.experimental.pallas import tpu as pltpu
from jax.sharding import PartitionSpec as P

REACH = 4
MASKED = -1e30
LOG2E = 1.4426950408889634
MESH = pl.DeviceIdType.MESH
NT = (((1,), (1,)), ((), ()))


def kernel(
    nk,
    nt,
    bias_ref,
    lse_ref,
    k_ref,
    v_ref,
    q_hbm,
    do_hbm,
    x_hbm,
    qg_ref,
    kg_ref,
    vg_ref,
    wg_ref,
    q_s,
    do_s,
    x_s,
    q6,
    do6,
    kw,
    vw,
    kt,
    own_bias,
    p_s,
    pb_s,
    ds_s,
    dvo,
    dvi,
    dko,
    dki,
    dv_own,
    x_t,
    x_in,
    vpair,
    po,
    ri,
    ld_sem,
    k_send,
    k_recv,
    v_send,
    v_recv,
    dv_send,
    dv_recv,
    dk_send,
    dk_recv,
    x_send,
    x_recv,
    x_loc,
    vp_send,
    vp_recv,
    rs_send,
    rs_recv,
):
    me = lax.axis_index("kv")
    tp = lax.axis_index("tp")
    core = lax.rem(me, 2)
    chip = me // 2
    sib = me + 1 - 2 * core
    chips = nk // 2
    tok, hd = k_ref.shape
    heads = lse_ref.shape[0]
    nblk = bias_ref.shape[1]
    blk = tok // nblk
    scale = hd**-0.5
    per_tp, _, rw, _ = x_t.shape

    loads = [
        pltpu.make_async_copy(src, dst, ld_sem.at[i])
        for i, (src, dst) in enumerate(((x_hbm, x_s), (q_hbm, q_s), (do_hbm, do_s)))
    ]
    for load in loads:
        load.start()

    barrier = pltpu.get_barrier_semaphore()

    @pl.loop(1, nk)
    def _(j):
        pl.semaphore_signal(
            barrier, inc=1, device_id=(lax.rem(me + j, nk), tp), device_id_type=MESH
        )

    for dt in range(1, nt):
        for kv in (me, sib):
            pl.semaphore_signal(
                barrier, inc=1, device_id=(kv, lax.rem(tp + dt, nt)), device_id_type=MESH
            )
    pl.semaphore_wait(barrier, nk - 1 + 2 * (nt - 1))

    def remote(src, dst, send, recv, kv, t=None):
        return pltpu.make_async_remote_copy(
            src_ref=src,
            dst_ref=dst,
            send_sem=send,
            recv_sem=recv,
            device_id=(kv, tp if t is None else t),
            device_id_type=MESH,
        )

    def k_copy(o):
        return remote(k_ref, kw.at[o], k_send.at[o], k_recv.at[o], me + o)

    def v_copy(o):
        return remote(v_ref, vw.at[o], v_send.at[o], v_recv.at[o], me + o)

    def dv_copy(o):
        return remote(dvo.at[o], dvi.at[o], dv_send.at[o], dv_recv.at[o], me - o)

    def dk_copy(o):
        return remote(dko.at[o], dki.at[o], dk_send.at[o], dk_recv.at[o], me - o)

    for copy in (k_copy, v_copy):
        for o in range(1, REACH + 1):

            @pl.when(me + o < nk)
            def _():
                copy(o).start()

    loads[0].wait()
    x_t[...] = x_s[...].T.reshape(x_t.shape)
    x_copies = [
        remote(x_t.at[:, 1 - core], x_in.at[tp, core], x_send.at[0, 1], x_recv.at[tp, core], sib)
    ]
    for dt in range(1, nt):
        other = lax.rem(tp + dt, nt)
        for s, kv, par in ((0, me, core), (1, sib, 1 - core)):
            x_copies.append(
                remote(
                    x_t.at[:, par],
                    x_in.at[tp, core],
                    x_send.at[dt, s],
                    x_recv.at[tp, core],
                    kv,
                    other,
                )
            )
    for copy in x_copies:
        copy.start()
    x_local = pltpu.make_async_copy(x_t.at[:, core], x_in.at[tp, core], x_loc)
    x_local.start()

    zero = jnp.zeros((tok, hd), jnp.bfloat16)
    for o in range(1, REACH + 1):

        @pl.when(me < o)
        def _():
            kw[o] = zero
            vw[o] = zero

        @pl.when(me + o >= nk)
        def _():
            dvi[o] = zero
            dki[o] = zero

    kw[0] = k_ref[...]
    vw[0] = v_ref[...]
    loads[1].wait()
    loads[2].wait()
    for a in range(heads):
        q6[a] = q_s[:, a * hd : (a + 1) * hd]
        do6[a] = do_s[:, a * hd : (a + 1) * hd]
    key_row = lax.broadcasted_iota(jnp.int32, (blk, tok), 0)
    pos = lax.broadcasted_iota(jnp.int32, (blk, tok), 1)
    for j in range(nblk):
        own_bias[j * blk : (j + 1) * blk, :] = jnp.where(
            key_row + j * blk > pos, MASKED, bias_ref[0, j : j + 1, :]
        )

    def first(o, own):
        keys = kw[o]
        for a in range(heads):
            s = lax.dot_general(keys, q6[a], NT, preferred_element_type=jnp.float32)
            s = s * (scale * LOG2E)
            lse = lse_ref[a : a + 1, :] * LOG2E
            if own:
                p = jnp.exp2(s + (own_bias[...] - lse))
            else:
                rows = bias_ref[o] - lse
                p = jnp.exp2(s.reshape(nblk, blk, tok) + rows[:, None, :]).reshape(tok, tok)
            p_s[a, o] = p
            pb_s[:, a * tok : (a + 1) * tok] = p.astype(jnp.bfloat16)
        return jnp.dot(
            pb_s[...], do6[...].reshape(heads * tok, hd), preferred_element_type=jnp.float32
        )

    dv_own[...] = first(0, True)

    @pl.loop(1, REACH + 1)
    def _(o):
        @pl.when(me >= o)
        def _():
            k_copy(o).wait_recv()

        dvo[o] = first(o, False).astype(jnp.bfloat16)

        @pl.when(me >= o)
        def _():
            dv_copy(o).start()

    kt[...] = kw[...].reshape((REACH + 1) * tok, hd).T
    for o in range(1, REACH + 1):

        @pl.when(me >= o)
        def _():
            v_copy(o).wait_recv()

    for a in range(heads):
        gw = lax.dot_general(
            vw[...].reshape((REACH + 1) * tok, hd), do6[a], NT, preferred_element_type=jnp.float32
        )
        p = p_s[a].reshape((REACH + 1) * tok, tok)
        delta = jnp.sum(p * gw, 0, keepdims=True)
        ds = (p * (gw - delta)).astype(jnp.bfloat16)
        ds_s[:, a * tok : (a + 1) * tok] = ds
        dq_t = jnp.dot(kt[...], ds, preferred_element_type=jnp.float32) * scale
        qg_ref[:, a * hd : (a + 1) * hd] = dq_t.T.astype(jnp.bfloat16)

    value = dv_own[...]
    for o in range(1, REACH + 1):

        @pl.when(me + o < nk)
        def _():
            dv_copy(o).wait_recv()

        value = value + dvi[o].astype(jnp.float32)
    value = value.astype(jnp.bfloat16)
    vg_ref[...] = value
    vpair[pl.ds(core, 1)] = value[None]
    pair = remote(vpair.at[core], vpair.at[core], vp_send, vp_recv, sib)
    pair.start()

    dk = (
        jnp.dot(ds_s[...], q6[...].reshape(heads * tok, hd), preferred_element_type=jnp.float32)
        * scale
    )
    dko[...] = dk.astype(jnp.bfloat16).reshape(REACH + 1, tok, hd)

    x_local.wait()
    for t in range(nt):
        for c in range(2):

            @pl.when((t != tp) | (c != core))
            def _():
                remote(
                    x_t.at[:, 0], x_in.at[t, c], x_send.at[0, 1], x_recv.at[t, c], sib
                ).wait_recv()

    remote(
        vpair.at[core], vpair.at[1 - core], vp_send, vp_recv, sib
    ).wait_recv()
    for t in range(nt):
        part = jnp.dot(
            x_in[t, 0].reshape(per_tp * rw, tok), vpair[0], preferred_element_type=jnp.float32
        ) + jnp.dot(
            x_in[t, 1].reshape(per_tp * rw, tok), vpair[1], preferred_element_type=jnp.float32
        )
        po[t * per_tp : (t + 1) * per_tp] = part.astype(jnp.bfloat16).reshape(per_tp, rw, hd)

    def rs_copy(j):
        to = lax.rem(chip + j, chips)
        return remote(po.at[to], ri.at[chip], rs_send.at[j], rs_recv.at[chip], to * 2 + core)

    @pl.loop(1, chips)
    def _(j):
        rs_copy(j).start()

    for o in range(1, REACH + 1):

        @pl.when(me >= o)
        def _():
            dk_copy(o).start()

    ri[pl.ds(chip, 1)] = po[pl.ds(chip, 1)]
    key = dk[:tok]
    for o in range(1, REACH + 1):

        @pl.when(me + o < nk)
        def _():
            dk_copy(o).wait_recv()

        key = key + dki[o].astype(jnp.float32)
    kg_ref[...] = key.astype(jnp.bfloat16)

    @pl.loop(1, chips)
    def _(j):
        src = lax.rem(chip + j, chips)
        remote(po.at[src], ri.at[src], rs_send.at[j], rs_recv.at[src], src * 2 + core).wait_recv()

    wg_ref[...] = jnp.sum(ri[...].astype(jnp.float32), 0)

    for o in range(1, REACH + 1):

        @pl.when(me + o < nk)
        def _():
            k_copy(o).wait_send()
            v_copy(o).wait_send()

        @pl.when(me >= o)
        def _():
            dv_copy(o).wait_send()
            dk_copy(o).wait_send()

    for copy in x_copies:
        copy.wait_send()
    pair.wait_send()

    @pl.loop(1, chips)
    def _(j):
        rs_copy(j).wait_send()


def shards(nk, nt, queries, keys, values, log_sums, out_grad, chosen, inputs):
    tok, hd = keys.shape
    heads = queries.shape[1] // hd
    nblk = chosen.shape[0]
    blk = tok // nblk
    feats = inputs.shape[1]
    rw = feats * nt // nk
    per_tp = feats // (2 * rw)
    span = REACH + 1
    device = lax.axis_index("kv")
    listed = chosen[:, 0, :]
    own_ids = device * nblk + jnp.arange(nblk, dtype=jnp.int32)
    win_ids = (
        (device - jnp.arange(span, dtype=jnp.int32)[:, None]) * nblk
        + jnp.arange(nblk, dtype=jnp.int32)[None, :]
    ).reshape(span * nblk)
    hit = (listed[None] == win_ids[:, None, None]) & (listed < own_ids[:, None])[None]
    allowed = jnp.any(hit, 2) | (win_ids[:, None] == own_ids[None, :])
    bias = jnp.repeat(jnp.where(allowed, 0.0, MASKED).astype(jnp.float32), blk, axis=1)
    bias = bias.reshape(span, nblk, tok)

    bf, f32 = jnp.bfloat16, jnp.float32
    dma = pltpu.SemaphoreType.DMA
    vmem = pl.BlockSpec(memory_space=pltpu.VMEM)
    hbm = pl.BlockSpec(memory_space=pl.ANY)
    return pl.pallas_call(
        functools.partial(kernel, nk, nt),
        out_shape=(
            jax.ShapeDtypeStruct((tok, heads * hd), bf),
            jax.ShapeDtypeStruct((tok, hd), bf),
            jax.ShapeDtypeStruct((tok, hd), bf),
            jax.ShapeDtypeStruct((rw, hd), f32),
        ),
        in_specs=[vmem, vmem, vmem, vmem, hbm, hbm, hbm],
        out_specs=(vmem, vmem, vmem, vmem),
        scratch_shapes=[
            pltpu.VMEM((tok, heads * hd), bf),
            pltpu.VMEM((tok, heads * hd), bf),
            pltpu.VMEM((tok, feats), bf),
            pltpu.VMEM((heads, tok, hd), bf),
            pltpu.VMEM((heads, tok, hd), bf),
            pltpu.VMEM((span, tok, hd), bf),
            pltpu.VMEM((span, tok, hd), bf),
            pltpu.VMEM((hd, span * tok), bf),
            pltpu.VMEM((tok, tok), f32),
            pltpu.VMEM((heads, span, tok, tok), f32),
            pltpu.VMEM((tok, heads * tok), bf),
            pltpu.VMEM((span * tok, heads * tok), bf),
            pltpu.VMEM((span, tok, hd), bf),
            pltpu.VMEM((span, tok, hd), bf),
            pltpu.VMEM((span, tok, hd), bf),
            pltpu.VMEM((span, tok, hd), bf),
            pltpu.VMEM((tok, hd), f32),
            pltpu.VMEM((per_tp, 2, rw, tok), bf),
            pltpu.VMEM((nt, 2, per_tp, rw, tok), bf),
            pltpu.VMEM((2, tok, hd), bf),
            pltpu.VMEM((nk // 2, rw, hd), bf),
            pltpu.VMEM((nk // 2, rw, hd), bf),
            dma((3,)),
            dma((span,)),
            dma((span,)),
            dma((span,)),
            dma((span,)),
            dma((span,)),
            dma((span,)),
            dma((span,)),
            dma((span,)),
            dma((nt, 2)),
            dma((nt, 2)),
            dma,
            dma,
            dma,
            dma((nk // 2,)),
            dma((nk // 2,)),
        ],
        compiler_params=pltpu.CompilerParams(
            collective_id=0, has_side_effects=True, vmem_limit_bytes=60 * 1024 * 1024
        ),
    )(bias, log_sums, keys, values, queries, out_grad, inputs)


def solution(mesh):
    in_specs = (
        P("kv", "tp"),
        P("kv", "tp"),
        P("kv", "tp"),
        P("tp", "kv"),
        P("kv", "tp"),
        P("kv", "tp", None),
        P("kv", "tp"),
    )
    out_specs = (P("kv", "tp"), P("kv", "tp"), P("kv", "tp"), P("kv", "tp"))
    return jax.shard_map(
        functools.partial(shards, mesh.shape["kv"], mesh.shape["tp"]),
        mesh=mesh,
        in_specs=in_specs,
        out_specs=out_specs,
        check_vma=False,
    )
```

```python
import functools

import jax
import jax.numpy as jnp
from jax import lax
from jax.experimental import pallas as pl
from jax.experimental.pallas import tpu as pltpu
from jax.sharding import PartitionSpec as P

REACH = 4
MASKED = -1e30
LOG2E = 1.4426950408889634
MESH = pl.DeviceIdType.MESH
NT = (((1,), (1,)), ((), ()))


def kernel(
    nk,
    nt,
    chosen_ref,
    lse_ref,
    k_ref,
    v_ref,
    q_hbm,
    do_hbm,
    x_hbm,
    qg_ref,
    kg_ref,
    vg_ref,
    wg_ref,
    q_s,
    do_s,
    x_s,
    q6,
    do6,
    kw,
    vw,
    kt,
    bias_ref,
    own_bias,
    p_s,
    pb_s,
    ds_s,
    dvo,
    dvi,
    dko,
    dki,
    dv_own,
    x_t,
    x_in,
    vpair,
    po,
    ri,
    ld_sem,
    k_send,
    k_recv,
    v_send,
    v_recv,
    dv_send,
    dv_recv,
    dk_send,
    dk_recv,
    x_send,
    x_recv,
    x_loc,
    vp_send,
    vp_recv,
    rs_send,
    rs_recv,
):
    me = lax.axis_index("kv")
    tp = lax.axis_index("tp")
    core = lax.rem(me, 2)
    chip = me // 2
    sib = me + 1 - 2 * core
    chips = nk // 2
    tok, hd = k_ref.shape
    heads = lse_ref.shape[0]
    nblk = chosen_ref.shape[0]
    blk = tok // nblk
    scale = hd**-0.5
    per_tp, _, rw, _ = x_t.shape

    loads = [
        pltpu.make_async_copy(src, dst, ld_sem.at[i])
        for i, (src, dst) in enumerate(((x_hbm, x_s), (q_hbm, q_s), (do_hbm, do_s)))
    ]
    for load in loads:
        load.start()

    barrier = pltpu.get_barrier_semaphore()

    @pl.loop(1, nk)
    def _(j):
        pl.semaphore_signal(
            barrier, inc=1, device_id=(lax.rem(me + j, nk), tp), device_id_type=MESH
        )

    for dt in range(1, nt):
        for kv in (me, sib):
            pl.semaphore_signal(
                barrier, inc=1, device_id=(kv, lax.rem(tp + dt, nt)), device_id_type=MESH
            )
    pl.semaphore_wait(barrier, nk - 1 + 2 * (nt - 1))

    def remote(src, dst, send, recv, kv, t=None):
        return pltpu.make_async_remote_copy(
            src_ref=src,
            dst_ref=dst,
            send_sem=send,
            recv_sem=recv,
            device_id=(kv, tp if t is None else t),
            device_id_type=MESH,
        )

    def k_copy(o):
        return remote(k_ref, kw.at[o], k_send.at[o], k_recv.at[o], me + o)

    def v_copy(o):
        return remote(v_ref, vw.at[o], v_send.at[o], v_recv.at[o], me + o)

    def dv_copy(o):
        return remote(dvo.at[o], dvi.at[o], dv_send.at[o], dv_recv.at[o], me - o)

    def dk_copy(o):
        return remote(dko.at[o], dki.at[o], dk_send.at[o], dk_recv.at[o], me - o)

    for copy in (k_copy, v_copy):
        for o in range(1, REACH + 1):

            @pl.when(me + o < nk)
            def _():
                copy(o).start()

    loads[0].wait()
    x_t[...] = x_s[...].T.reshape(x_t.shape)
    half = per_tp // 2
    x_copies = []
    for h in range(2):
        rows = pl.ds(h * half, half)
        for dt in range(1, nt):
            other = lax.rem(tp + dt, nt)
            for s, kv, par in ((0, me, core), (1, sib, 1 - core)):
                x_copies.append(
                    remote(
                        x_t.at[rows, par],
                        x_in.at[tp, core, rows],
                        x_send.at[h, dt, s],
                        x_recv.at[h, tp, core],
                        kv,
                        other,
                    )
                )
        x_copies.append(
            remote(
                x_t.at[rows, 1 - core],
                x_in.at[tp, core, rows],
                x_send.at[h, 0, 1],
                x_recv.at[h, tp, core],
                sib,
            )
        )
    for copy in x_copies:
        copy.start()
    x_local = pltpu.make_async_copy(x_t.at[:, core], x_in.at[tp, core], x_loc)
    x_local.start()

    zero = jnp.zeros((tok, hd), jnp.bfloat16)
    for o in range(1, REACH + 1):

        @pl.when(me < o)
        def _():
            kw[o] = zero
            vw[o] = zero

        @pl.when(me + o >= nk)
        def _():
            dvi[o] = zero
            dki[o] = zero

    kw[0] = k_ref[...]
    vw[0] = v_ref[...]
    loads[1].wait()
    loads[2].wait()
    for a in range(heads):
        q6[a] = q_s[:, a * hd : (a + 1) * hd]
        do6[a] = do_s[:, a * hd : (a + 1) * hd]
    row = lax.broadcasted_iota(jnp.int32, (nblk, tok), 0)
    col = lax.broadcasted_iota(jnp.int32, (nblk, tok), 1)
    marked = [jnp.full((nblk, tok), MASKED, jnp.float32) for _ in range(REACH + 1)]
    for b in range(nblk):
        in_block = (col >= b * blk) & (col < (b + 1) * blk)
        marked[0] = jnp.where(in_block & (row == b), 0.0, marked[0])
        for slot in range(chosen_ref.shape[2]):
            block = chosen_ref[b, 0, slot]
            block = jnp.where(block < me * nblk + b, block, -1)
            for o in range(REACH + 1):
                hit = in_block & (row + (me - o) * nblk == block)
                marked[o] = jnp.where(hit & (block >= 0), 0.0, marked[o])
    for o in range(REACH + 1):
        bias_ref[o] = marked[o]
    key_row = lax.broadcasted_iota(jnp.int32, (blk, tok), 0)
    pos = lax.broadcasted_iota(jnp.int32, (blk, tok), 1)
    for j in range(nblk):
        own_bias[j * blk : (j + 1) * blk, :] = jnp.where(
            key_row + j * blk > pos, MASKED, bias_ref[0, j : j + 1, :]
        )

    def first(o, own):
        keys = kw[o]
        for a in range(heads):
            s = lax.dot_general(keys, q6[a], NT, preferred_element_type=jnp.float32)
            s = s * (scale * LOG2E)
            lse = lse_ref[a : a + 1, :] * LOG2E
            if own:
                p = jnp.exp2(s + (own_bias[...] - lse))
            else:
                rows = bias_ref[o] - lse
                p = jnp.exp2(s.reshape(nblk, blk, tok) + rows[:, None, :]).reshape(tok, tok)
            p_s[a, o] = p
            pb_s[:, a * tok : (a + 1) * tok] = p.astype(jnp.bfloat16)
        return jnp.dot(
            pb_s[...], do6[...].reshape(heads * tok, hd), preferred_element_type=jnp.float32
        )

    dv_own[...] = first(0, True)

    @pl.loop(1, REACH + 1)
    def _(o):
        @pl.when(me >= o)
        def _():
            k_copy(o).wait_recv()

        dvo[o] = first(o, False).astype(jnp.bfloat16)

        @pl.when(me >= o)
        def _():
            dv_copy(o).start()

    kt[...] = kw[...].reshape((REACH + 1) * tok, hd).T
    for o in range(1, REACH + 1):

        @pl.when(me >= o)
        def _():
            v_copy(o).wait_recv()

    def score_grad(a):
        gw = lax.dot_general(
            vw[...].reshape((REACH + 1) * tok, hd), do6[a], NT, preferred_element_type=jnp.float32
        )
        p = p_s[a].reshape((REACH + 1) * tok, tok)
        delta = jnp.sum(p * gw, 0, keepdims=True)
        ds_s[:, a * tok : (a + 1) * tok] = (p * (gw - delta)).astype(jnp.bfloat16)

    def query_part(a):
        ds = ds_s[:, a * tok : (a + 1) * tok]
        dq_t = jnp.dot(kt[...], ds, preferred_element_type=jnp.float32) * scale
        qg_ref[:, a * hd : (a + 1) * hd] = dq_t.T.astype(jnp.bfloat16)

    def rs_copy(to):
        return remote(po.at[to], ri.at[chip], rs_send.at[to], rs_recv.at[chip], to * 2 + core)

    def weight_part(dt, h):
        t = lax.rem(tp + dt, nt)
        rows = pl.ds(h * half, half)
        for c in range(2):

            @pl.when((t != tp) | (c != core))
            def _():
                remote(
                    x_t.at[rows, 0],
                    x_in.at[t, c, rows],
                    x_send.at[0, 0, 1],
                    x_recv.at[h, t, c],
                    sib,
                ).wait_recv()

        part = jnp.dot(
            x_in[t, 0, rows].reshape(half * rw, tok), vpair[0], preferred_element_type=jnp.float32
        ) + jnp.dot(
            x_in[t, 1, rows].reshape(half * rw, tok), vpair[1], preferred_element_type=jnp.float32
        )
        start = t * per_tp + h * half
        po[pl.ds(start, half)] = part.astype(jnp.bfloat16).reshape(half, rw, hd)

        @pl.loop(0, half)
        def _(j):
            @pl.when(start + j != chip)
            def _():
                rs_copy(start + j).start()

    split = heads // 2
    for a in range(split):
        score_grad(a)

    value = dv_own[...]
    for o in range(1, REACH + 1):

        @pl.when(me + o < nk)
        def _():
            dv_copy(o).wait_recv()

        value = value + dvi[o].astype(jnp.float32)
    value = value.astype(jnp.bfloat16)
    vg_ref[...] = value
    vpair[pl.ds(core, 1)] = value[None]
    pair = remote(vpair.at[core], vpair.at[core], vp_send, vp_recv, sib)
    pair.start()
    score_grad(split)
    remote(vpair.at[core], vpair.at[1 - core], vp_send, vp_recv, sib).wait_recv()
    x_local.wait()
    for dt in range(1, nt):
        weight_part(dt, 0)
    for h in range(2):
        weight_part(0, h)
    for a in range(split + 1, heads):
        score_grad(a)

    for o in range(REACH, -1, -1):
        dk = (
            jnp.dot(
                ds_s[o * tok : (o + 1) * tok, :],
                q6[...].reshape(heads * tok, hd),
                preferred_element_type=jnp.float32,
            )
            * scale
        )
        if o == 0:
            key = dk
        else:
            dko[o] = dk.astype(jnp.bfloat16)

            @pl.when(me >= o)
            def _():
                dk_copy(o).start()

    for a in range(split):
        query_part(a)
    for dt in range(1, nt):
        weight_part(dt, 1)
    for a in range(split, heads):
        query_part(a)

    ri[pl.ds(chip, 1)] = po[pl.ds(chip, 1)]
    for o in range(1, REACH + 1):

        @pl.when(me + o < nk)
        def _():
            dk_copy(o).wait_recv()

        key = key + dki[o].astype(jnp.float32)
    kg_ref[...] = key.astype(jnp.bfloat16)

    @pl.loop(1, chips)
    def _(j):
        src = lax.rem(chip + j, chips)
        remote(po.at[src], ri.at[src], rs_send.at[src], rs_recv.at[src], src * 2 + core).wait_recv()

    wg_ref[...] = jnp.sum(ri[...].astype(jnp.float32), 0)

    for o in range(1, REACH + 1):

        @pl.when(me + o < nk)
        def _():
            k_copy(o).wait_send()
            v_copy(o).wait_send()

        @pl.when(me >= o)
        def _():
            dv_copy(o).wait_send()
            dk_copy(o).wait_send()

    for copy in x_copies:
        copy.wait_send()
    pair.wait_send()

    @pl.loop(1, chips)
    def _(j):
        rs_copy(lax.rem(chip + j, chips)).wait_send()


def finish(*refs):
    count = len(refs) // 2
    sems = refs[-1]
    copies = [
        pltpu.make_async_copy(refs[i], refs[count + i], sems.at[i]) for i in range(count)
    ]
    for copy in copies:
        copy.start()
    for copy in copies:
        copy.wait()


def shards(nk, nt, queries, keys, values, log_sums, out_grad, chosen, inputs):
    tok, hd = keys.shape
    heads = queries.shape[1] // hd
    nblk = chosen.shape[0]
    feats = inputs.shape[1]
    rw = feats * nt // nk
    per_tp = feats // (2 * rw)
    span = REACH + 1
    bf, f32 = jnp.bfloat16, jnp.float32
    dma = pltpu.SemaphoreType.DMA
    vmem = pl.BlockSpec(memory_space=pltpu.VMEM)
    hbm = pl.BlockSpec(memory_space=pl.ANY)
    parts = pl.pallas_call(
        functools.partial(kernel, nk, nt),
        out_shape=(
            jax.ShapeDtypeStruct((tok, heads * hd), bf),
            jax.ShapeDtypeStruct((tok, hd), bf),
            jax.ShapeDtypeStruct((tok, hd), bf),
            jax.ShapeDtypeStruct((rw, hd), f32),
        ),
        in_specs=[pl.BlockSpec(memory_space=pltpu.SMEM), vmem, vmem, vmem, hbm, hbm, hbm],
        out_specs=(vmem, vmem, vmem, vmem),
        scratch_shapes=[
            pltpu.VMEM((tok, heads * hd), bf),
            pltpu.VMEM((tok, heads * hd), bf),
            pltpu.VMEM((tok, feats), bf),
            pltpu.VMEM((heads, tok, hd), bf),
            pltpu.VMEM((heads, tok, hd), bf),
            pltpu.VMEM((span, tok, hd), bf),
            pltpu.VMEM((span, tok, hd), bf),
            pltpu.VMEM((hd, span * tok), bf),
            pltpu.VMEM((span, nblk, tok), f32),
            pltpu.VMEM((tok, tok), f32),
            pltpu.VMEM((heads, span, tok, tok), f32),
            pltpu.VMEM((tok, heads * tok), bf),
            pltpu.VMEM((span * tok, heads * tok), bf),
            pltpu.VMEM((span, tok, hd), bf),
            pltpu.VMEM((span, tok, hd), bf),
            pltpu.VMEM((span, tok, hd), bf),
            pltpu.VMEM((span, tok, hd), bf),
            pltpu.VMEM((tok, hd), f32),
            pltpu.VMEM((per_tp, 2, rw, tok), bf),
            pltpu.VMEM((nt, 2, per_tp, rw, tok), bf),
            pltpu.VMEM((2, tok, hd), bf),
            pltpu.VMEM((nk // 2, rw, hd), bf),
            pltpu.VMEM((nk // 2, rw, hd), bf),
            dma((3,)),
            dma((span,)),
            dma((span,)),
            dma((span,)),
            dma((span,)),
            dma((span,)),
            dma((span,)),
            dma((span,)),
            dma((span,)),
            dma((2, nt, 2)),
            dma((2, nt, 2)),
            dma,
            dma,
            dma,
            dma((nk // 2,)),
            dma((nk // 2,)),
        ],
        compiler_params=pltpu.CompilerParams(
            collective_id=0, has_side_effects=True, vmem_limit_bytes=60 * 1024 * 1024
        ),
    )(chosen, log_sums, keys, values, queries, out_grad, inputs)
    return pl.pallas_call(
        finish,
        out_shape=tuple(jax.ShapeDtypeStruct(part.shape, part.dtype) for part in parts),
        in_specs=[vmem] * len(parts),
        out_specs=(hbm,) * len(parts),
        scratch_shapes=[dma((len(parts),))],
    )(*parts)


def solution(mesh):
    in_specs = (
        P("kv", "tp"),
        P("kv", "tp"),
        P("kv", "tp"),
        P("tp", "kv"),
        P("kv", "tp"),
        P("kv", "tp", None),
        P("kv", "tp"),
    )
    out_specs = (P("kv", "tp"), P("kv", "tp"), P("kv", "tp"), P("kv", "tp"))
    return jax.shard_map(
        functools.partial(shards, mesh.shape["kv"], mesh.shape["tp"]),
        mesh=mesh,
        in_specs=in_specs,
        out_specs=out_specs,
        check_vma=False,
    )
```

```python
import functools

import jax
import jax.numpy as jnp
from jax import lax
from jax.experimental import pallas as pl
from jax.experimental.pallas import tpu as pltpu
from jax.sharding import PartitionSpec as P

REACH = 4
MASKED = -1e30
LOG2E = 1.4426950408889634
MESH = pl.DeviceIdType.MESH
NT = (((1,), (1,)), ((), ()))


def kernel(
    nk,
    nt,
    chosen_ref,
    lse_ref,
    k_ref,
    v_ref,
    q_hbm,
    do_hbm,
    x_hbm,
    qg_ref,
    kg_ref,
    vg_ref,
    wg_ref,
    q_s,
    do_s,
    x_s,
    q6,
    do6,
    kw,
    vw,
    kt,
    bias_ref,
    own_bias,
    p_s,
    pb_s,
    ds_s,
    dvo,
    dvi,
    dko,
    dki,
    dv_sum,
    dk_sum,
    dv_out,
    dv_in,
    dk_out,
    dk_in,
    x_t,
    x_in,
    vpair,
    po,
    ri,
    ld_sem,
    own_sem,
    k_send,
    k_recv,
    v_send,
    v_recv,
    dv_send,
    dv_recv,
    dk_send,
    dk_recv,
    x_send,
    x_recv,
    x_loc,
    vp_send,
    vp_recv,
    rs_send,
    rs_recv,
):
    me = lax.axis_index("kv")
    tp = lax.axis_index("tp")
    core = lax.rem(me, 2)
    chip = me // 2
    sib = me + 1 - 2 * core
    chips = nk // 2
    tok, hd = k_ref.shape
    heads = lse_ref.shape[0]
    nblk = chosen_ref.shape[0]
    blk = tok // nblk
    scale = hd**-0.5
    per_tp, _, rw, _ = x_t.shape

    loads = [
        pltpu.make_async_copy(src, dst, ld_sem.at[i])
        for i, (src, dst) in enumerate(((x_hbm, x_s), (q_hbm, q_s), (do_hbm, do_s)))
    ]
    for load in loads:
        load.start()

    barrier = pltpu.get_barrier_semaphore()

    @pl.loop(1, nk)
    def _(j):
        pl.semaphore_signal(
            barrier, inc=1, device_id=(lax.rem(me + j, nk), tp), device_id_type=MESH
        )

    for dt in range(1, nt):
        for kv in (me, sib):
            pl.semaphore_signal(
                barrier, inc=1, device_id=(kv, lax.rem(tp + dt, nt)), device_id_type=MESH
            )
    pl.semaphore_wait(barrier, nk - 1 + 2 * (nt - 1))

    def remote(src, dst, send, recv, kv, t=None):
        return pltpu.make_async_remote_copy(
            src_ref=src,
            dst_ref=dst,
            send_sem=send,
            recv_sem=recv,
            device_id=(kv, tp if t is None else t),
            device_id_type=MESH,
        )

    def k_copy(o):
        return remote(k_ref, kw.at[o], k_send.at[o], k_recv.at[o], me + o)

    def v_copy(o):
        return remote(v_ref, vw.at[o], v_send.at[o], v_recv.at[o], me + o)

    def dv_copy(o):
        return remote(dvo.at[o], dvi.at[o], dv_send.at[o], dv_recv.at[o], me - o)

    def dk_copy(o):
        return remote(dko.at[o], dki.at[o], dk_send.at[o], dk_recv.at[o], me - o)

    def k_pass(u):
        src = kw.at[2 * u + 2 * core]
        return remote(src, kw.at[2 * u + 1], k_send.at[2 * u + 1], k_recv.at[2 * u + 1], sib)

    def v_pass(u):
        src = vw.at[2 * u + 2 * core]
        return remote(src, vw.at[2 * u + 1], v_send.at[2 * u + 1], v_recv.at[2 * u + 1], sib)

    def dv_hand(u):
        return remote(
            dv_out.at[u], dv_in.at[u], dv_send.at[2 * u + 1], dv_recv.at[2 * u + 1], sib
        )

    def dk_hand(u):
        return remote(
            dk_out.at[u], dk_in.at[u], dk_send.at[2 * u + 1], dk_recv.at[2 * u + 1], sib
        )

    def take_hands(hand, landed, sums):
        for u in range(2):

            @pl.when(me >= 2 * u + 2 * core)
            def _():
                hand(u).wait_recv()
                slot = pl.ds(u + core, 1)
                sums[slot] = sums[slot] + landed[u][None].astype(jnp.float32)

    for copy in (k_copy, v_copy):
        for o in (2, 4):

            @pl.when(me + o < nk)
            def _():
                copy(o).start()

    loads[0].wait()
    x_t[...] = x_s[...].T.reshape(x_t.shape)
    half = per_tp // 2
    x_copies = []
    for h in range(2):
        rows = pl.ds(h * half, half)
        for dt in range(1, nt):
            other = lax.rem(tp + dt, nt)
            for s, kv, par in ((0, me, core), (1, sib, 1 - core)):
                x_copies.append(
                    remote(
                        x_t.at[rows, par],
                        x_in.at[tp, core, rows],
                        x_send.at[h, dt, s],
                        x_recv.at[h, tp, core],
                        kv,
                        other,
                    )
                )
        x_copies.append(
            remote(
                x_t.at[rows, 1 - core],
                x_in.at[tp, core, rows],
                x_send.at[h, 0, 1],
                x_recv.at[h, tp, core],
                sib,
            )
        )
    for copy in x_copies:
        copy.start()
    x_local = pltpu.make_async_copy(x_t.at[:, core], x_in.at[tp, core], x_loc)
    x_local.start()

    zero = jnp.zeros((tok, hd), jnp.bfloat16)
    for o in range(1, REACH + 1):

        @pl.when(me < o)
        def _():
            kw[o] = zero
            vw[o] = zero

        @pl.when(me + o >= nk)
        def _():
            dvi[o] = zero
            dki[o] = zero

    own = [
        pltpu.make_async_copy(src, dst.at[0], own_sem.at[n])
        for n, (src, dst) in enumerate(((k_ref, kw), (v_ref, vw)))
    ]
    for copy in own:
        copy.start()
    for copy in own:
        copy.wait()

    @pl.when(core == 0)
    def _():
        k_pass(0).start()
        v_pass(0).start()

    loads[1].wait()
    loads[2].wait()
    for a in range(heads):
        q6[a] = q_s[:, a * hd : (a + 1) * hd]
        do6[a] = do_s[:, a * hd : (a + 1) * hd]
    row = lax.broadcasted_iota(jnp.int32, (nblk, tok), 0)
    col = lax.broadcasted_iota(jnp.int32, (nblk, tok), 1)
    marked = [jnp.full((nblk, tok), MASKED, jnp.float32) for _ in range(REACH + 1)]
    for b in range(nblk):
        in_block = (col >= b * blk) & (col < (b + 1) * blk)
        marked[0] = jnp.where(in_block & (row == b), 0.0, marked[0])
        for slot in range(chosen_ref.shape[2]):
            block = chosen_ref[b, 0, slot]
            block = jnp.where(block < me * nblk + b, block, -1)
            for o in range(REACH + 1):
                hit = in_block & (row + (me - o) * nblk == block)
                marked[o] = jnp.where(hit & (block >= 0), 0.0, marked[o])
    for o in range(REACH + 1):
        bias_ref[o] = marked[o]
    key_row = lax.broadcasted_iota(jnp.int32, (blk, tok), 0)
    pos = lax.broadcasted_iota(jnp.int32, (blk, tok), 1)
    for j in range(nblk):
        own_bias[j * blk : (j + 1) * blk, :] = jnp.where(
            key_row + j * blk > pos, MASKED, bias_ref[0, j : j + 1, :]
        )

    def first(o, own):
        keys = kw[o]
        for a in range(heads):
            s = lax.dot_general(keys, q6[a], NT, preferred_element_type=jnp.float32)
            s = s * (scale * LOG2E)
            lse = lse_ref[a : a + 1, :] * LOG2E
            if own:
                p = jnp.exp2(s + (own_bias[...] - lse))
            else:
                rows = bias_ref[o] - lse
                p = jnp.exp2(s.reshape(nblk, blk, tok) + rows[:, None, :]).reshape(tok, tok)
            p_s[a, o] = p
            pb_s[:, a * tok : (a + 1) * tok] = p.astype(jnp.bfloat16)
        return jnp.dot(
            pb_s[...], do6[...].reshape(heads * tok, hd), preferred_element_type=jnp.float32
        )

    dv_sum[0] = first(0, True)

    @pl.loop(0, 2)
    def _(u):
        @pl.when(me >= 2 * u + 2)
        def _():
            k_copy(2 * u + 2).wait_recv()

            @pl.when((u == 0) | (core == 1))
            def _():
                k_pass(jnp.where(u == 0, 1 - core, 1)).start()

        dv_sum[u + 1] = first(2 * u + 2, False)

        @pl.when(me >= 2 * u + 1)
        def _():
            k_pass(u).wait_recv()

        dv_out[u] = first(2 * u + 1, False).astype(jnp.bfloat16)

        @pl.when(me >= 2 * u + 1)
        def _():
            dv_hand(u).start()

    for u in range(2):

        @pl.when(me >= 2 * u + 2)
        def _():
            v_copy(2 * u + 2).wait_recv()

            @pl.when((u == 0) | (core == 1))
            def _():
                v_pass(jnp.where(u == 0, 1 - core, 1)).start()

    kt[...] = kw[...].reshape((REACH + 1) * tok, hd).T
    take_hands(dv_hand, dv_in, dv_sum)
    for o in (4, 2):
        dvo[o] = dv_sum[o // 2].astype(jnp.bfloat16)

        @pl.when(me >= o)
        def _():
            dv_copy(o).start()

    for u in range(2):

        @pl.when(me >= 2 * u + 1)
        def _():
            v_pass(u).wait_recv()

    def score_grad(a):
        gw = lax.dot_general(
            vw[...].reshape((REACH + 1) * tok, hd), do6[a], NT, preferred_element_type=jnp.float32
        )
        p = p_s[a].reshape((REACH + 1) * tok, tok)
        delta = jnp.sum(p * gw, 0, keepdims=True)
        ds_s[:, a * tok : (a + 1) * tok] = (p * (gw - delta)).astype(jnp.bfloat16)

    def query_part(a):
        ds = ds_s[:, a * tok : (a + 1) * tok]
        dq_t = jnp.dot(kt[...], ds, preferred_element_type=jnp.float32) * scale
        qg_ref[:, a * hd : (a + 1) * hd] = dq_t.T.astype(jnp.bfloat16)

    def rs_copy(to):
        return remote(po.at[to], ri.at[chip], rs_send.at[to], rs_recv.at[chip], to * 2 + core)

    def weight_part(dt, h):
        t = lax.rem(tp + dt, nt)
        rows = pl.ds(h * half, half)
        for c in range(2):

            @pl.when((t != tp) | (c != core))
            def _():
                remote(
                    x_t.at[rows, 0],
                    x_in.at[t, c, rows],
                    x_send.at[0, 0, 1],
                    x_recv.at[h, t, c],
                    sib,
                ).wait_recv()

        part = jnp.dot(
            x_in[t, 0, rows].reshape(half * rw, tok), vpair[0], preferred_element_type=jnp.float32
        ) + jnp.dot(
            x_in[t, 1, rows].reshape(half * rw, tok), vpair[1], preferred_element_type=jnp.float32
        )
        start = t * per_tp + h * half
        po[pl.ds(start, half)] = part.astype(jnp.bfloat16).reshape(half, rw, hd)

        @pl.loop(0, half)
        def _(j):
            @pl.when(start + j != chip)
            def _():
                rs_copy(start + j).start()

    split = heads // 2
    for a in range(split):
        score_grad(a)

    value = dv_sum[0]
    for o in (2, 4):

        @pl.when(me + o < nk)
        def _():
            dv_copy(o).wait_recv()

        value = value + dvi[o].astype(jnp.float32)
    value = value.astype(jnp.bfloat16)
    vg_ref[...] = value
    vpair[pl.ds(core, 1)] = value[None]
    pair = remote(vpair.at[core], vpair.at[core], vp_send, vp_recv, sib)
    pair.start()
    score_grad(split)
    remote(vpair.at[core], vpair.at[1 - core], vp_send, vp_recv, sib).wait_recv()
    x_local.wait()
    for h in range(2):
        for dt in range(nt - 1, -1, -1):
            weight_part(dt, h)
    for a in range(split + 1, heads):
        score_grad(a)

    for o in (3, 1, 4, 2, 0):
        dk = (
            jnp.dot(
                ds_s[o * tok : (o + 1) * tok, :],
                q6[...].reshape(heads * tok, hd),
                preferred_element_type=jnp.float32,
            )
            * scale
        )
        if o % 2 == 0:
            dk_sum[o // 2] = dk
        else:
            dk_out[o // 2] = dk.astype(jnp.bfloat16)

            @pl.when(me >= o)
            def _():
                dk_hand(o // 2).start()

    take_hands(dk_hand, dk_in, dk_sum)
    for o in (4, 2):
        dko[o] = dk_sum[o // 2].astype(jnp.bfloat16)

        @pl.when(me >= o)
        def _():
            dk_copy(o).start()

    for a in range(heads):
        query_part(a)

    key = dk_sum[0]
    ri[pl.ds(chip, 1)] = po[pl.ds(chip, 1)]
    for o in (2, 4):

        @pl.when(me + o < nk)
        def _():
            dk_copy(o).wait_recv()

        key = key + dki[o].astype(jnp.float32)
    kg_ref[...] = key.astype(jnp.bfloat16)

    @pl.loop(1, chips)
    def _(j):
        src = lax.rem(chip + j, chips)
        remote(po.at[src], ri.at[src], rs_send.at[src], rs_recv.at[src], src * 2 + core).wait_recv()

    wg_ref[...] = jnp.sum(ri[...].astype(jnp.float32), 0)

    for o in (2, 4):

        @pl.when(me + o < nk)
        def _():
            k_copy(o).wait_send()
            v_copy(o).wait_send()

        @pl.when(me >= o)
        def _():
            dv_copy(o).wait_send()
            dk_copy(o).wait_send()

    for u in range(2):

        @pl.when(me >= 2 * u + 2 * core)
        def _():
            k_pass(u).wait_send()
            v_pass(u).wait_send()

        @pl.when(me >= 2 * u + 1)
        def _():
            dv_hand(u).wait_send()
            dk_hand(u).wait_send()

    for copy in x_copies:
        copy.wait_send()
    pair.wait_send()

    @pl.loop(1, chips)
    def _(j):
        rs_copy(lax.rem(chip + j, chips)).wait_send()


def finish(*refs):
    count = len(refs) // 2
    sems = refs[-1]
    copies = [
        pltpu.make_async_copy(refs[i], refs[count + i], sems.at[i]) for i in range(count)
    ]
    for copy in copies:
        copy.start()
    for copy in copies:
        copy.wait()


def shards(nk, nt, queries, keys, values, log_sums, out_grad, chosen, inputs):
    tok, hd = keys.shape
    heads = queries.shape[1] // hd
    nblk = chosen.shape[0]
    feats = inputs.shape[1]
    rw = feats * nt // nk
    per_tp = feats // (2 * rw)
    span = REACH + 1
    bf, f32 = jnp.bfloat16, jnp.float32
    dma = pltpu.SemaphoreType.DMA
    vmem = pl.BlockSpec(memory_space=pltpu.VMEM)
    hbm = pl.BlockSpec(memory_space=pl.ANY)
    parts = pl.pallas_call(
        functools.partial(kernel, nk, nt),
        out_shape=(
            jax.ShapeDtypeStruct((tok, heads * hd), bf),
            jax.ShapeDtypeStruct((tok, hd), bf),
            jax.ShapeDtypeStruct((tok, hd), bf),
            jax.ShapeDtypeStruct((rw, hd), f32),
        ),
        in_specs=[pl.BlockSpec(memory_space=pltpu.SMEM), vmem, vmem, vmem, hbm, hbm, hbm],
        out_specs=(vmem, vmem, vmem, vmem),
        scratch_shapes=[
            pltpu.VMEM((tok, heads * hd), bf),
            pltpu.VMEM((tok, heads * hd), bf),
            pltpu.VMEM((tok, feats), bf),
            pltpu.VMEM((heads, tok, hd), bf),
            pltpu.VMEM((heads, tok, hd), bf),
            pltpu.VMEM((span, tok, hd), bf),
            pltpu.VMEM((span, tok, hd), bf),
            pltpu.VMEM((hd, span * tok), bf),
            pltpu.VMEM((span, nblk, tok), f32),
            pltpu.VMEM((tok, tok), f32),
            pltpu.VMEM((heads, span, tok, tok), f32),
            pltpu.VMEM((tok, heads * tok), bf),
            pltpu.VMEM((span * tok, heads * tok), bf),
            pltpu.VMEM((span, tok, hd), bf),
            pltpu.VMEM((span, tok, hd), bf),
            pltpu.VMEM((span, tok, hd), bf),
            pltpu.VMEM((span, tok, hd), bf),
            pltpu.VMEM((3, tok, hd), f32),
            pltpu.VMEM((3, tok, hd), f32),
            pltpu.VMEM((2, tok, hd), bf),
            pltpu.VMEM((2, tok, hd), bf),
            pltpu.VMEM((2, tok, hd), bf),
            pltpu.VMEM((2, tok, hd), bf),
            pltpu.VMEM((per_tp, 2, rw, tok), bf),
            pltpu.VMEM((nt, 2, per_tp, rw, tok), bf),
            pltpu.VMEM((2, tok, hd), bf),
            pltpu.VMEM((nk // 2, rw, hd), bf),
            pltpu.VMEM((nk // 2, rw, hd), bf),
            dma((3,)),
            dma((2,)),
            dma((span,)),
            dma((span,)),
            dma((span,)),
            dma((span,)),
            dma((span,)),
            dma((span,)),
            dma((span,)),
            dma((span,)),
            dma((2, nt, 2)),
            dma((2, nt, 2)),
            dma,
            dma,
            dma,
            dma((nk // 2,)),
            dma((nk // 2,)),
        ],
        compiler_params=pltpu.CompilerParams(
            collective_id=0, has_side_effects=True, vmem_limit_bytes=60 * 1024 * 1024
        ),
    )(chosen, log_sums, keys, values, queries, out_grad, inputs)
    return pl.pallas_call(
        finish,
        out_shape=tuple(jax.ShapeDtypeStruct(part.shape, part.dtype) for part in parts),
        in_specs=[vmem] * len(parts),
        out_specs=(hbm,) * len(parts),
        scratch_shapes=[dma((len(parts),))],
    )(*parts)


def solution(mesh):
    in_specs = (
        P("kv", "tp"),
        P("kv", "tp"),
        P("kv", "tp"),
        P("tp", "kv"),
        P("kv", "tp"),
        P("kv", "tp", None),
        P("kv", "tp"),
    )
    out_specs = (P("kv", "tp"), P("kv", "tp"), P("kv", "tp"), P("kv", "tp"))
    return jax.shard_map(
        functools.partial(shards, mesh.shape["kv"], mesh.shape["tp"]),
        mesh=mesh,
        in_specs=in_specs,
        out_specs=out_specs,
        check_vma=False,
    )
```
